32 devices in a mesh: sp: 4 (over z), fs: 4 (over y, core), tp: 2 (over x).
Axes of the slice: x: 2, y: 2, z: 4, core: 2. Of those that a mesh axis runs over, the one named last changes fastest.
Arguments:
- tokens: bfloat16 [8, 2048, 2048], P('fs', ('sp', 'tp')), may hold values from -6 to 6
- norm_gain: float32 [2048], replicated, may hold values from 0.1 to 1.9
- w_pool_in: bfloat16 [2048, 1024], P('fs', 'tp'), may hold values from -0.125 to 0.125
- pool_mix: bfloat16 [8, 128, 128], replicated, may hold values from -0.5 to 0.5
- pool_scale: float32 [1024], replicated, may hold values from 0.1 to 1.9
- w_query: bfloat16 [2048, 1024], P('fs', 'tp'), may hold values from -0.13258252 to 0.13258252
- w_key: bfloat16 [2048, 1024], P('fs', 'tp'), may hold values from -0.508233 to 0.508233
- w_value: bfloat16 [2048, 1024], P('fs', 'tp'), may hold values from -0.125 to 0.125
- gate_cache: float32 [8, 8, 2048], P('fs', 'tp'), may hold values from -258 to 0, as said below
- w_out_pool: bfloat16 [1024, 2048], P('tp', 'fs'), may hold values from -0.125 to 0.125
- w_out_attn: bfloat16 [1024, 2048], P('tp', 'fs'), may hold values from -0.75 to 0.75
Outputs:
- mixed: bfloat16 [8, 2048, 2048], P('fs', ('sp', 'tp'))
The draws below stay inside these ranges and needn't reach their ends.
Inputs may be any that keep to these rules, and one draw needn't show every extreme that they name: `gate_cache`: each head's values never rise along the positions.
All inputs are finite; a program needn't handle non-finite values.
Results may differ from the reference program's by a relative error of at most 0.014.
Values may be sent and summed in bfloat16 or wider, within the bound.
A program may use at most 128 MiB of HBM per device.

```python
import jax
import jax.numpy as jnp
from jax import lax

D = 2048
HEAD_DIM = 128
HEAD_TOTAL = 8
GROUPS = 8
GROUP_WIDTH = 128
POOL_WIDTH = 1024
ATTN_WIDTH = 1024
TOK_DEV = 512
SEQUENCE_LENGTH = 2048
SEQUENCE_TOTAL = 8
N_TP = 2


def query_key_pair(key):
    joined = jax.random.fold_in(key, 4242)
    first_key, second_key = jax.random.split(joined)
    query_part = jnp.clip(jax.random.normal(first_key, (D, ATTN_WIDTH), jnp.float32), -6.0, 6.0)
    key_part = jnp.clip(jax.random.normal(second_key, (D, ATTN_WIDTH), jnp.float32), -6.0, 6.0)
    return (query_part * D ** (-0.5), key_part * D ** (-0.5))


def draw_w_query(key, part):
    return query_key_pair(key)[0].astype(jnp.bfloat16)


def draw_w_key(key, part):
    return query_key_pair(key)[1].astype(jnp.bfloat16)


def draw_gate_cache(key, part):
    joined = jax.random.fold_in(key, 917)
    sequence_flows = jax.random.split(joined, 7)
    block_count = SEQUENCE_LENGTH // TOK_DEV
    ranking = jax.vmap(lambda single: jax.random.permutation(single, HEAD_TOTAL))(jax.random.split(sequence_flows[0], SEQUENCE_TOTAL))
    fast_count = HEAD_TOTAL // 2
    rapid_decay = ranking < fast_count
    quick_rate = jnp.exp(jax.random.uniform(sequence_flows[1], (SEQUENCE_TOTAL, HEAD_TOTAL), jnp.float32, jnp.log(1.0 / 100.0), jnp.log(1.0 / 30.0)))
    slow_total = jnp.exp(jax.random.uniform(sequence_flows[2], (SEQUENCE_TOTAL, HEAD_TOTAL), jnp.float32, jnp.log(0.15), jnp.log(0.5)))
    baseline_rate = jnp.where(rapid_decay, quick_rate, slow_total / SEQUENCE_LENGTH)
    block_factor = jnp.exp(jax.random.uniform(sequence_flows[3], (SEQUENCE_TOTAL, HEAD_TOTAL, block_count), jnp.float32, jnp.log(0.5), jnp.log(2.0)))
    position_multiplier = jnp.repeat(block_factor, TOK_DEV, axis=2)
    jitter_level = jax.random.uniform(sequence_flows[4], (SEQUENCE_TOTAL, HEAD_TOTAL, SEQUENCE_LENGTH), jnp.float32, 0.2, 1.8)
    spike_locations = jax.random.randint(sequence_flows[5], (SEQUENCE_TOTAL, HEAD_TOTAL, 2), 0, SEQUENCE_LENGTH)
    spike_depth = jax.random.uniform(sequence_flows[6], (SEQUENCE_TOTAL, HEAD_TOTAL, 2), jnp.float32, 0.22, 0.6)
    token_positions = jnp.arange(SEQUENCE_LENGTH)
    spike_hits = token_positions[None, None, None, :] == spike_locations[:, :, :, None]
    spike_events = jnp.sum(jnp.where(spike_hits, spike_depth[:, :, :, None], 0.0), axis=2)
    spike_events = jnp.where(rapid_decay[:, :, None], 0.0, spike_events)
    step_increments = baseline_rate[:, :, None] * position_multiplier * jitter_level + spike_events
    return -jnp.cumsum(step_increments, axis=2)


def block_scale(own_key, extent, shards, smallest, top_value):
    def one(dim, shards_of):
        steps = jax.random.uniform(jax.random.fold_in(jax.random.fold_in(own_key, 6), dim), (shards_of,), jnp.float32, smallest / len(shards), top_value / len(shards))
        return jnp.repeat(jnp.exp(steps), extent[dim] // shards_of).reshape((-1,) + (1,) * (len(extent) - dim - 1))

    gain = one(*shards[0])
    for cut in shards[1:]:
        gain = gain * one(*cut)
    return gain


def centred(rng, extent, scale, most, cuts=(), kind=jnp.bfloat16):
    result = jax.random.normal(rng, extent, jnp.float32) * scale
    if len(cuts) > 0:
        result = block_scale(rng, extent, cuts, -0.22, 0.18) * result
    return jnp.clip(result, min=-most, max=most).astype(kind)


def setup_inputs(seed: int = 0) -> dict:
    key_of = jax.random.split(jax.random.key(seed), 12)
    return {
        "tokens": centred(key_of[0], (SEQUENCE_TOTAL, SEQUENCE_LENGTH, D), 1.0, 6.0, ((0, 4), (1, 8))),
        "norm_gain": jnp.clip(1.0 + 0.18 * jax.random.normal(key_of[1], (D,), jnp.float32), 0.1, 1.9),
        "w_pool_in": centred(key_of[2], (D, POOL_WIDTH), D ** -0.5, 0.125, ((0, 4), (1, 2))),
        "pool_mix": centred(key_of[3], (GROUPS, GROUP_WIDTH, GROUP_WIDTH), GROUP_WIDTH ** -0.5, 0.5),
        "pool_scale": jnp.clip(1.0 + 0.18 * jax.random.normal(key_of[4], (POOL_WIDTH,), jnp.float32), 0.1, 1.9),
        "w_query": draw_w_query(jax.random.fold_in(key_of[11], 71), 0),
        "w_key": draw_w_key(jax.random.fold_in(key_of[11], 71), 0),
        "w_value": centred(key_of[7], (D, ATTN_WIDTH), D ** -0.5, 0.125, ((0, 4), (1, 2))),
        "gate_cache": draw_gate_cache(jax.random.fold_in(key_of[11], 71), 0),
        "w_out_pool": centred(key_of[9], (POOL_WIDTH, D), (POOL_WIDTH + ATTN_WIDTH) ** -0.5, 0.125, ((0, 2), (1, 4))),
        "w_out_attn": centred(key_of[10], (ATTN_WIDTH, D), (ATTN_WIDTH // 16) ** -0.5, 0.75, ((0, 2), (1, 4))),
    }


norm_eps = 1e-06
widest = 16

def settle(values):
    return lax.optimization_barrier(values.astype(jnp.bfloat16))

def window_sums(extended):
    outcome = []
    current = extended
    offset = 1
    for doubling in range(4):
        padding = jnp.zeros((offset, extended.shape[1]), extended.dtype)
        current = current + jnp.concatenate([padding, current[:-offset]], axis=0)
        offset = offset * 2
        outcome.append(current[widest - 1:])
    return outcome

def pool_branch(projected, mixing, scaling):
    row_count = projected.shape[0]
    channels = projected.shape[1]
    border = jnp.zeros((widest - 1, channels), jnp.float32)
    widened = projected.astype(jnp.float32)
    totals = window_sums(jnp.concatenate([border, widened], axis=0))
    token_positions = jnp.arange(row_count)
    window_index = jnp.arange(channels) // GROUP_WIDTH % 4
    averaged = jnp.zeros((row_count, channels), jnp.float32)
    for doubling in range(4):
        counted = jnp.minimum(token_positions + 1, 2 ** (doubling + 1)).astype(jnp.float32)
        picked = (window_index == doubling).astype(jnp.float32)
        averaged = averaged + picked[None, :] * totals[doubling] / counted[:, None]
    departure = settle(averaged - widened).astype(jnp.float32)
    mixed_rows = jnp.einsum('tgc,gcd->tgd', departure.reshape(row_count, GROUPS, GROUP_WIDTH), mixing.astype(jnp.float32))
    return (mixed_rows.reshape(row_count, channels) * scaling[None, :]).astype(jnp.bfloat16)

def attention(query_proj, key_proj, value_proj, gate_rows):
    row_count = query_proj.shape[0]
    block_rows = 512 if row_count % 512 == 0 else row_count
    shaped = (row_count, HEAD_TOTAL, HEAD_DIM)
    query_heads = query_proj.reshape(shaped).astype(jnp.float32)
    key_heads = key_proj.reshape(shaped).astype(jnp.float32)
    value_heads = value_proj.reshape(shaped).astype(jnp.float32)
    gate_cols = jnp.transpose(gate_rows)
    pieces = []
    for query_start in range(0, row_count, block_rows):
        query_end = query_start + block_rows
        scores = jnp.einsum('qhd,khd->qhk', query_heads[query_start:query_end], key_heads[:query_end]) * HEAD_DIM ** (-0.5)
        scores = scores + gate_cols[query_start:query_end, :, None] - gate_rows[None, :, :query_end]
        allowed = (jnp.arange(query_end)[None, :] <= jnp.arange(query_start, query_end)[:, None])[:, None, :]
        scores = jnp.where(allowed, scores, -jnp.inf)
        highest = lax.optimization_barrier(jnp.max(scores, axis=2, keepdims=True))
        lifted = jnp.exp(scores - highest)
        denominator = lax.optimization_barrier(jnp.sum(lifted, axis=2))
        rounded = settle(lifted).astype(jnp.float32)
        weighted = jnp.einsum('qhk,khd->qhd', rounded, value_heads[:query_end])
        pieces.append((weighted / denominator[:, :, None]).astype(jnp.bfloat16))
    return jnp.concatenate(pieces, axis=0).reshape(row_count, HEAD_TOTAL * HEAD_DIM)

def reference(tokens, norm_gain, w_pool_in, pool_mix, pool_scale, w_query, w_key, w_value, gate_cache, w_out_pool, w_out_attn):
    pool_share = POOL_WIDTH // N_TP
    attn_share = ATTN_WIDTH // N_TP
    outputs = []
    for sequence in range(SEQUENCE_TOTAL):
        widened = tokens[sequence].astype(jnp.float32)
        normed = (widened * lax.rsqrt(lax.optimization_barrier(jnp.mean(widened * widened, axis=-1, keepdims=True)) + norm_eps) * norm_gain[None, :]).astype(jnp.bfloat16)
        pool_in = settle(jnp.dot(normed, w_pool_in, preferred_element_type=jnp.float32))
        query_proj = settle(jnp.dot(normed, w_query, preferred_element_type=jnp.float32))
        key_proj = settle(jnp.dot(normed, w_key, preferred_element_type=jnp.float32))
        value_proj = settle(jnp.dot(normed, w_value, preferred_element_type=jnp.float32))
        pool_out = pool_branch(pool_in, pool_mix, pool_scale)
        attn_out = attention(query_proj, key_proj, value_proj, gate_cache[sequence])
        summed = jnp.zeros((SEQUENCE_LENGTH, D), jnp.float32)
        for member in range(N_TP):
            pool_lo = member * pool_share
            attn_lo = member * attn_share
            partial_value = jnp.dot(pool_out[:, pool_lo:pool_lo + pool_share], w_out_pool[pool_lo:pool_lo + pool_share], preferred_element_type=jnp.float32)
            partial_value = partial_value + jnp.dot(attn_out[:, attn_lo:attn_lo + attn_share], w_out_attn[attn_lo:attn_lo + attn_share], preferred_element_type=jnp.float32)
            summed = summed + settle(partial_value).astype(jnp.float32)
        outputs.append(summed.astype(jnp.bfloat16))
    return jnp.stack(outputs, axis=0)
```

```python
import jax
import jax.numpy as jnp
from jax import lax
from jax.experimental import pallas as pl
from jax.experimental.pallas import tpu as pltpu
from jax.sharding import PartitionSpec as P

HEAD_DIM = 128
GROUP_WIDTH = 128


norm_eps = 1e-06
widest = 16
masked_score = -1e30


def shifted(x, axis, by):
    length = lax.axis_size(axis)
    pairs = [(i, i + by) for i in range(length) if 0 <= i + by < length]
    return lax.ppermute(x, axis, pairs)


def window_sums(extended):
    outcome = []
    current = extended
    offset = 1
    for doubling in range(4):
        padding = jnp.zeros((offset, extended.shape[1]), jnp.float32)
        current = current + jnp.concatenate([padding, current[:-offset]], axis=0)
        offset = offset * 2
        outcome.append(current[widest - 1 :])
    return outcome


def pool_branch(projected, border, first_group, first_position, mixing, scaling):
    row_count = projected.shape[0]
    channels = projected.shape[1]
    widened = projected.astype(jnp.float32)
    totals = window_sums(jnp.concatenate([border.astype(jnp.float32), widened], axis=0))
    token_positions = first_position + jnp.arange(row_count)
    window_index = (first_group + jnp.arange(channels) // GROUP_WIDTH) % 4
    averaged = jnp.zeros((row_count, channels), jnp.float32)
    for doubling in range(4):
        counted = jnp.minimum(token_positions + 1, 2 ** (doubling + 1)).astype(jnp.float32)
        picked = (window_index == doubling).astype(jnp.float32)
        averaged = averaged + picked[None, :] * totals[doubling] / counted[:, None]
    departure = (averaged - widened).astype(jnp.bfloat16)
    group_count = channels // GROUP_WIDTH
    mixed_rows = jnp.einsum(
        "tgc,gcd->tgd",
        departure.reshape(row_count, group_count, GROUP_WIDTH),
        mixing,
        preferred_element_type=jnp.float32,
    )
    return (mixed_rows.reshape(row_count, channels) * scaling[None, :]).astype(jnp.bfloat16)


def general_device(
    tokens,
    norm_gain,
    w_pool_in,
    pool_mix,
    pool_scale,
    w_query,
    w_key,
    w_value,
    gate_cache,
    w_out_pool,
    w_out_attn,
):
    tp_index = lax.axis_index("tp")
    tp_count = lax.axis_size("tp")
    seq_count = tokens.shape[0]
    own_count = tokens.shape[1]
    token_count = own_count * tp_count
    first_position = lax.axis_index("sp") * token_count
    own_rows = tokens.astype(jnp.float32)
    normed = (
        own_rows
        * lax.rsqrt(jnp.mean(own_rows * own_rows, axis=-1, keepdims=True) + norm_eps)
        * norm_gain[None, None, :]
    ).astype(jnp.bfloat16)
    pool_full, query_full, key_full, value_full, out_pool_full, out_attn_full = (
        lax.all_gather(w_pool_in, "fs", axis=0, tiled=True),
        lax.all_gather(w_query, "fs", axis=0, tiled=True),
        lax.all_gather(w_key, "fs", axis=0, tiled=True),
        lax.all_gather(w_value, "fs", axis=0, tiled=True),
        lax.all_gather(w_out_pool, "fs", axis=1, tiled=True),
        lax.all_gather(w_out_attn, "fs", axis=1, tiled=True),
    )
    pool_cols = w_pool_in.shape[1]
    attn_cols = w_query.shape[1]
    shard_rows = lax.all_gather(normed, "tp", axis=1, tiled=True)
    projected = jnp.concatenate(
        [
            jnp.dot(shard_rows, pool_full, preferred_element_type=jnp.float32).astype(jnp.bfloat16),
            jnp.dot(shard_rows, query_full, preferred_element_type=jnp.float32).astype(
                jnp.bfloat16
            ),
            jnp.dot(shard_rows, key_full, preferred_element_type=jnp.float32).astype(jnp.bfloat16),
            jnp.dot(shard_rows, value_full, preferred_element_type=jnp.float32).astype(
                jnp.bfloat16
            ),
        ],
        axis=2,
    )
    pool_in = projected[:, :, :pool_cols]
    query_proj = projected[:, :, pool_cols : pool_cols + attn_cols]
    key_proj = projected[:, :, pool_cols + attn_cols : pool_cols + 2 * attn_cols]
    value_proj = projected[:, :, pool_cols + 2 * attn_cols :]
    group_local = pool_cols // GROUP_WIDTH
    mixing = lax.dynamic_slice_in_dim(pool_mix, tp_index * group_local, group_local, 0)
    scaling = lax.dynamic_slice_in_dim(pool_scale, tp_index * pool_cols, pool_cols, 0)
    borders = shifted(pool_in[:, token_count - (widest - 1) :], "sp", 1)
    pool_out = jnp.stack(
        [
            pool_branch(
                pool_in[member],
                borders[member],
                tp_index * group_local,
                first_position,
                mixing,
                scaling,
            )
            for member in range(seq_count)
        ],
        axis=0,
    )
    head_count = attn_cols // HEAD_DIM
    query_heads = query_proj.reshape(seq_count, token_count, head_count, HEAD_DIM)
    query_gates = jnp.transpose(
        lax.dynamic_slice_in_dim(gate_cache, first_position, token_count, 2), (0, 2, 1)
    )
    query_positions = first_position + jnp.arange(token_count)
    last_position = first_position + token_count - 1
    score_scale = HEAD_DIM ** (-0.5)
    start_state = (
        jnp.full((seq_count, token_count, head_count), masked_score, jnp.float32),
        jnp.zeros((seq_count, token_count, head_count), jnp.float32),
        jnp.zeros((seq_count, token_count, head_count, HEAD_DIM), jnp.float32),
    )
    key_shard = lax.all_gather(key_proj, "sp", axis=1, tiled=True)
    value_shard = lax.all_gather(value_proj, "sp", axis=1, tiled=True)
    key_total = key_shard.shape[1]
    block_rows = 512

    def one_block(block_state, block_index):
        key_start = block_index * block_rows

        def compute(inner_state):
            running_top, running_sum, running_out = inner_state
            key_block = lax.dynamic_slice_in_dim(key_shard, block_index * block_rows, block_rows, 1)
            value_block = lax.dynamic_slice_in_dim(
                value_shard, block_index * block_rows, block_rows, 1
            )
            key_block = key_block.reshape(seq_count, block_rows, head_count, HEAD_DIM)
            value_block = value_block.reshape(seq_count, block_rows, head_count, HEAD_DIM)
            key_gates = lax.dynamic_slice_in_dim(gate_cache, key_start, block_rows, 2)
            scores = (
                jnp.einsum(
                    "sqhd,skhd->sqhk", query_heads, key_block, preferred_element_type=jnp.float32
                )
                * score_scale
            )
            scores = scores + query_gates[:, :, :, None] - key_gates[:, None, :, :]
            allowed = ((key_start + jnp.arange(block_rows))[None, :] <= query_positions[:, None])[
                None, :, None, :
            ]
            scores = jnp.where(allowed, scores, masked_score)
            new_top = jnp.maximum(running_top, jnp.max(scores, axis=3))
            weights = jnp.where(allowed, jnp.exp(scores - new_top[:, :, :, None]), 0.0)
            shrink = jnp.exp(running_top - new_top)
            running_sum = running_sum * shrink + jnp.sum(weights, axis=3)
            running_out = running_out * shrink[:, :, :, None] + jnp.einsum(
                "sqhk,skhd->sqhd",
                weights.astype(jnp.bfloat16),
                value_block,
                preferred_element_type=jnp.float32,
            )
            return (new_top, running_sum, running_out)

        def unchanged(inner_state):
            return inner_state

        return (lax.cond(key_start <= last_position, compute, unchanged, block_state), None)

    result, unused = lax.scan(one_block, start_state, jnp.arange(key_total // block_rows))
    final_top, final_sum, final_out = result
    attn_out = (
        (final_out / final_sum[:, :, :, None])
        .astype(jnp.bfloat16)
        .reshape(seq_count, token_count, attn_cols)
    )
    pool_flat = jnp.transpose(
        pool_out.reshape(seq_count, tp_count, own_count, pool_cols), (1, 0, 2, 3)
    ).reshape(tp_count * seq_count * own_count, pool_cols)
    attn_flat = jnp.transpose(
        attn_out.reshape(seq_count, tp_count, own_count, attn_cols), (1, 0, 2, 3)
    ).reshape(tp_count * seq_count * own_count, attn_cols)
    summed = lax.psum_scatter(
        (
            jnp.dot(pool_flat, out_pool_full, preferred_element_type=jnp.float32)
            + jnp.dot(attn_flat, out_attn_full, preferred_element_type=jnp.float32)
        ).astype(jnp.bfloat16),
        "tp",
        scatter_dimension=0,
        tiled=True,
    ).astype(jnp.float32)
    return summed.astype(jnp.bfloat16).reshape(seq_count, own_count, summed.shape[1])


query_block = 512


def attention_kernel(packed_ref, column_ref, row_ref, out_ref, top_ref, sum_ref, total_ref):
    block = pl.program_id(0)
    start = pl.multiple_of(block * query_block, query_block)
    query = packed_ref[pl.ds(start, query_block), 0:HEAD_DIM]
    gate = column_ref[...]
    top_ref[...] = jnp.full(top_ref.shape, masked_score, jnp.float32)
    sum_ref[...] = jnp.zeros_like(sum_ref)
    total_ref[...] = jnp.zeros_like(total_ref)

    def visit(key_start, diagonal):
        keys = packed_ref[pl.ds(key_start, query_block), HEAD_DIM : 2 * HEAD_DIM]
        values = packed_ref[pl.ds(key_start, query_block), 2 * HEAD_DIM : 3 * HEAD_DIM]
        scores = lax.dot_general(
            query, keys, (((1,), (1,)), ((), ())), preferred_element_type=jnp.float32
        )
        scores = scores * HEAD_DIM ** (-0.5) + (gate - row_ref[:, pl.ds(key_start, query_block)])
        if diagonal:
            below = lax.broadcasted_iota(jnp.int32, scores.shape, 1) <= lax.broadcasted_iota(
                jnp.int32, scores.shape, 0
            )
            scores = jnp.where(below, scores, masked_score)
        old_top = top_ref[...]
        new_top = jnp.maximum(old_top, jnp.max(scores, axis=1, keepdims=True))
        shrink = jnp.exp(old_top - new_top)
        lifted = jnp.exp(scores - new_top)
        if diagonal:
            lifted = jnp.where(below, lifted, 0.0)
        top_ref[...] = new_top
        sum_ref[...] = sum_ref[...] * shrink + jnp.sum(lifted, axis=1, keepdims=True)
        total_ref[...] = total_ref[...] * shrink + jnp.dot(
            lifted.astype(jnp.bfloat16), values, preferred_element_type=jnp.float32
        )

    def body(step, carry):
        visit(pl.multiple_of(step * query_block, query_block), False)
        return carry

    lax.fori_loop(0, block, body, 0)
    visit(start, True)
    out_ref[...] = (total_ref[...] / sum_ref[...]).astype(jnp.bfloat16)


def attend(packed, gate):
    rows = packed.shape[0]
    return pl.pallas_call(
        attention_kernel,
        grid=(rows // query_block,),
        in_specs=[
            pl.BlockSpec((rows, 3 * HEAD_DIM), lambda i: (0, 0)),
            pl.BlockSpec((query_block, 1), lambda i: (i, 0)),
            pl.BlockSpec((1, rows), lambda i: (0, 0)),
        ],
        out_specs=pl.BlockSpec((query_block, HEAD_DIM), lambda i: (i, 0)),
        out_shape=jax.ShapeDtypeStruct((rows, HEAD_DIM), jnp.bfloat16),
        scratch_shapes=[
            pltpu.VMEM((query_block, 1), jnp.float32),
            pltpu.VMEM((query_block, 1), jnp.float32),
            pltpu.VMEM((query_block, HEAD_DIM), jnp.float32),
        ],
        cost_estimate=pl.CostEstimate(
            flops=2 * rows * rows * HEAD_DIM * 2,
            bytes_accessed=rows * HEAD_DIM * 8,
            transcendentals=rows * rows // 2,
        ),
        compiler_params=pltpu.CompilerParams(vmem_limit_bytes=32 * 1024 * 1024),
    )(packed, gate[:, None], gate[None, :])


def over_fs(own, fs_index):
    def flip(x, bit):
        return lax.ppermute(x, "fs", [(i, i ^ bit) for i in range(4)])

    sibling = flip(own, 1)
    across = flip(own, 2)
    corner = flip(across, 1)
    depth = own.shape[0]
    outcome = jnp.zeros((4 * depth, own.shape[1]), own.dtype)
    for mask, part in ((0, own), (1, sibling), (2, across), (3, corner)):
        outcome = lax.dynamic_update_slice_in_dim(
            outcome, part, jnp.bitwise_xor(fs_index, mask) * depth, 0
        )
    return outcome


def swap(x):
    return lax.ppermute(x, "tp", [(0, 1), (1, 0)])


def around(x, by):
    length = lax.axis_size("sp")
    return lax.ppermute(x, "sp", [(i, (i + by) % length) for i in range(length)])


def fast_device(
    tokens,
    norm_gain,
    w_pool_in,
    pool_mix,
    pool_scale,
    w_query,
    w_key,
    w_value,
    gate_cache,
    w_out_pool,
    w_out_attn,
):
    tp_index = lax.axis_index("tp")
    sp_index = lax.axis_index("sp")
    fs_index = lax.axis_index("fs")
    sp_count = lax.axis_size("sp")
    seq_count, own_count, width = tokens.shape
    token_count = 2 * own_count
    first_position = sp_index * token_count
    pool_cols = w_pool_in.shape[1]
    attn_cols = w_query.shape[1]
    group_local = pool_cols // GROUP_WIDTH
    others = [swap(tokens[s]) for s in range(seq_count)]
    query_key = over_fs(jnp.concatenate([w_query, w_key], axis=1), fs_index)
    value_pool = over_fs(jnp.concatenate([w_value, w_pool_in], axis=1), fs_index)
    out_own = jnp.concatenate([w_out_pool, w_out_attn], axis=0)
    out_all = (
        lax.all_gather(out_own, "fs", axis=0, tiled=False),
        lax.all_gather(swap(out_own), "fs", axis=0, tiled=False),
    )
    mixing = lax.dynamic_slice_in_dim(pool_mix, tp_index * group_local, group_local, 0)
    scaling = lax.dynamic_slice_in_dim(pool_scale, tp_index * pool_cols, pool_cols, 0)
    gates = lax.dynamic_index_in_dim(gate_cache, sp_index, 1, keepdims=False)

    def normalize(x):
        rows = x.astype(jnp.float32)
        return (
            rows
            * lax.rsqrt(jnp.mean(rows * rows, axis=-1, keepdims=True) + norm_eps)
            * norm_gain[None, :]
        ).astype(jnp.bfloat16)

    def project(rows, weights):
        return jnp.dot(rows, weights, preferred_element_type=jnp.float32).astype(jnp.bfloat16)

    arrived = []
    pooled = []
    for s in range(seq_count):
        mine = tokens[s]
        rows = normalize(
            jnp.concatenate(
                [
                    jnp.where(tp_index == 0, mine, others[s]),
                    jnp.where(tp_index == 0, others[s], mine),
                ],
                axis=0,
            )
        )
        first = project(rows, query_key)
        second = project(rows, value_pool)

        def message(dest):
            at = dest * HEAD_DIM
            return jnp.concatenate(
                [
                    lax.dynamic_slice_in_dim(first, at, HEAD_DIM, 1),
                    lax.dynamic_slice_in_dim(first, attn_cols + at, HEAD_DIM, 1),
                    lax.dynamic_slice_in_dim(second, at, HEAD_DIM, 1),
                ],
                axis=1,
            )

        packed = jnp.zeros((sp_count * token_count, 3 * HEAD_DIM), jnp.bfloat16)
        for by in range(sp_count):
            part = message((sp_index + by) % sp_count)
            if by > 0:
                part = around(part, by)
            packed = lax.dynamic_update_slice_in_dim(
                packed, part, ((sp_index + sp_count - by) % sp_count) * token_count, 0
            )
        arrived.append(packed)
        pool_in = second[:, attn_cols:]
        border = shifted(pool_in[token_count - (widest - 1) :], "sp", 1)
        pooled.append(
            pool_branch(
                pool_in, border, tp_index * group_local, first_position, mixing, scaling
            )
        )

    outputs = []
    for s in range(seq_count):
        attn = attend(arrived[s], gates[s])
        gathered = jnp.zeros((token_count, attn_cols), jnp.bfloat16)
        for by in range(sp_count):
            dest = (sp_index + by) % sp_count
            part = lax.dynamic_slice_in_dim(attn, dest * token_count, token_count, 0)
            if by > 0:
                part = around(part, by)
            gathered = lax.dynamic_update_slice_in_dim(
                gathered, part, ((sp_index + sp_count - by) % sp_count) * HEAD_DIM, 1
            )

        def halves(x):
            own = lax.dynamic_slice_in_dim(x, tp_index * own_count, own_count, 0)
            return own, swap(
                lax.dynamic_slice_in_dim(x, (1 - tp_index) * own_count, own_count, 0)
            )

        pool_own, pool_other = halves(pooled[s])
        attn_own, attn_other = halves(gathered)
        result = jnp.einsum(
            "mk,fkn->mfn",
            jnp.concatenate([pool_own, attn_own], axis=1),
            out_all[0],
            preferred_element_type=jnp.float32,
        ) + jnp.einsum(
            "mk,fkn->mfn",
            jnp.concatenate([pool_other, attn_other], axis=1),
            out_all[1],
            preferred_element_type=jnp.float32,
        )
        outputs.append(result.astype(jnp.bfloat16).reshape(own_count, width))
    return jnp.stack(outputs, axis=0)


def on_device(*args):
    heads = args[5].shape[1] // HEAD_DIM
    sp_count = lax.axis_size("sp")
    suited = lax.axis_size("tp") == 2 and lax.axis_size("fs") == 4 and heads == sp_count
    length = args[0].shape[1] * 2 * sp_count
    if suited and length % query_block == 0:
        return fast_device(*args)
    return general_device(*args)


def solution(mesh):
    placed = (
        P("fs", ("sp", "tp"), None),
        P(),
        P("fs", "tp"),
        P(),
        P(),
        P("fs", "tp"),
        P("fs", "tp"),
        P("fs", "tp"),
        P("fs", "tp", None),
        P("tp", "fs"),
        P("tp", "fs"),
    )
    return jax.shard_map(
        on_device,
        mesh=mesh,
        in_specs=placed,
        out_specs=P("fs", ("sp", "tp"), None),
        check_vma=False,
    )
```

```python
import jax
import jax.numpy as jnp
from jax import lax
from jax.experimental import pallas as pl
from jax.experimental.pallas import tpu as pltpu
from jax.sharding import PartitionSpec as P

HEAD_DIM = 128
GROUP_WIDTH = 128


norm_eps = 1e-06
widest = 16
masked_score = -1e30


def shifted(x, axis, by):
    length = lax.axis_size(axis)
    pairs = [(i, i + by) for i in range(length) if 0 <= i + by < length]
    return lax.ppermute(x, axis, pairs)


def window_sums(extended):
    outcome = []
    current = extended
    offset = 1
    for doubling in range(4):
        padding = jnp.zeros((offset, extended.shape[1]), jnp.float32)
        current = current + jnp.concatenate([padding, current[:-offset]], axis=0)
        offset = offset * 2
        outcome.append(current[widest - 1 :])
    return outcome


def pool_branch(projected, border, first_group, first_position, mixing, scaling):
    row_count = projected.shape[0]
    channels = projected.shape[1]
    widened = projected.astype(jnp.float32)
    totals = window_sums(jnp.concatenate([border.astype(jnp.float32), widened], axis=0))
    token_positions = first_position + jnp.arange(row_count)
    window_index = (first_group + jnp.arange(channels) // GROUP_WIDTH) % 4
    averaged = jnp.zeros((row_count, channels), jnp.float32)
    for doubling in range(4):
        counted = jnp.minimum(token_positions + 1, 2 ** (doubling + 1)).astype(jnp.float32)
        picked = (window_index == doubling).astype(jnp.float32)
        averaged = averaged + picked[None, :] * totals[doubling] / counted[:, None]
    departure = (averaged - widened).astype(jnp.bfloat16)
    group_count = channels // GROUP_WIDTH
    mixed_rows = jnp.einsum(
        "tgc,gcd->tgd",
        departure.reshape(row_count, group_count, GROUP_WIDTH),
        mixing,
        preferred_element_type=jnp.float32,
    )
    return (mixed_rows.reshape(row_count, channels) * scaling[None, :]).astype(jnp.bfloat16)


def general_device(
    tokens,
    norm_gain,
    w_pool_in,
    pool_mix,
    pool_scale,
    w_query,
    w_key,
    w_value,
    gate_cache,
    w_out_pool,
    w_out_attn,
):
    tp_index = lax.axis_index("tp")
    tp_count = lax.axis_size("tp")
    seq_count = tokens.shape[0]
    own_count = tokens.shape[1]
    token_count = own_count * tp_count
    first_position = lax.axis_index("sp") * token_count
    own_rows = tokens.astype(jnp.float32)
    normed = (
        own_rows
        * lax.rsqrt(jnp.mean(own_rows * own_rows, axis=-1, keepdims=True) + norm_eps)
        * norm_gain[None, None, :]
    ).astype(jnp.bfloat16)
    pool_full, query_full, key_full, value_full, out_pool_full, out_attn_full = (
        lax.all_gather(w_pool_in, "fs", axis=0, tiled=True),
        lax.all_gather(w_query, "fs", axis=0, tiled=True),
        lax.all_gather(w_key, "fs", axis=0, tiled=True),
        lax.all_gather(w_value, "fs", axis=0, tiled=True),
        lax.all_gather(w_out_pool, "fs", axis=1, tiled=True),
        lax.all_gather(w_out_attn, "fs", axis=1, tiled=True),
    )
    pool_cols = w_pool_in.shape[1]
    attn_cols = w_query.shape[1]
    shard_rows = lax.all_gather(normed, "tp", axis=1, tiled=True)
    projected = jnp.concatenate(
        [
            jnp.dot(shard_rows, pool_full, preferred_element_type=jnp.float32).astype(jnp.bfloat16),
            jnp.dot(shard_rows, query_full, preferred_element_type=jnp.float32).astype(
                jnp.bfloat16
            ),
            jnp.dot(shard_rows, key_full, preferred_element_type=jnp.float32).astype(jnp.bfloat16),
            jnp.dot(shard_rows, value_full, preferred_element_type=jnp.float32).astype(
                jnp.bfloat16
            ),
        ],
        axis=2,
    )
    pool_in = projected[:, :, :pool_cols]
    query_proj = projected[:, :, pool_cols : pool_cols + attn_cols]
    key_proj = projected[:, :, pool_cols + attn_cols : pool_cols + 2 * attn_cols]
    value_proj = projected[:, :, pool_cols + 2 * attn_cols :]
    group_local = pool_cols // GROUP_WIDTH
    mixing = lax.dynamic_slice_in_dim(pool_mix, tp_index * group_local, group_local, 0)
    scaling = lax.dynamic_slice_in_dim(pool_scale, tp_index * pool_cols, pool_cols, 0)
    borders = shifted(pool_in[:, token_count - (widest - 1) :], "sp", 1)
    pool_out = jnp.stack(
        [
            pool_branch(
                pool_in[member],
                borders[member],
                tp_index * group_local,
                first_position,
                mixing,
                scaling,
            )
            for member in range(seq_count)
        ],
        axis=0,
    )
    head_count = attn_cols // HEAD_DIM
    query_heads = query_proj.reshape(seq_count, token_count, head_count, HEAD_DIM)
    query_gates = jnp.transpose(
        lax.dynamic_slice_in_dim(gate_cache, first_position, token_count, 2), (0, 2, 1)
    )
    query_positions = first_position + jnp.arange(token_count)
    last_position = first_position + token_count - 1
    score_scale = HEAD_DIM ** (-0.5)
    start_state = (
        jnp.full((seq_count, token_count, head_count), masked_score, jnp.float32),
        jnp.zeros((seq_count, token_count, head_count), jnp.float32),
        jnp.zeros((seq_count, token_count, head_count, HEAD_DIM), jnp.float32),
    )
    key_shard = lax.all_gather(key_proj, "sp", axis=1, tiled=True)
    value_shard = lax.all_gather(value_proj, "sp", axis=1, tiled=True)
    key_total = key_shard.shape[1]
    block_rows = 512

    def one_block(block_state, block_index):
        key_start = block_index * block_rows

        def compute(inner_state):
            running_top, running_sum, running_out = inner_state
            key_block = lax.dynamic_slice_in_dim(key_shard, block_index * block_rows, block_rows, 1)
            value_block = lax.dynamic_slice_in_dim(
                value_shard, block_index * block_rows, block_rows, 1
            )
            key_block = key_block.reshape(seq_count, block_rows, head_count, HEAD_DIM)
            value_block = value_block.reshape(seq_count, block_rows, head_count, HEAD_DIM)
            key_gates = lax.dynamic_slice_in_dim(gate_cache, key_start, block_rows, 2)
            scores = (
                jnp.einsum(
                    "sqhd,skhd->sqhk", query_heads, key_block, preferred_element_type=jnp.float32
                )
                * score_scale
            )
            scores = scores + query_gates[:, :, :, None] - key_gates[:, None, :, :]
            allowed = ((key_start + jnp.arange(block_rows))[None, :] <= query_positions[:, None])[
                None, :, None, :
            ]
            scores = jnp.where(allowed, scores, masked_score)
            new_top = jnp.maximum(running_top, jnp.max(scores, axis=3))
            weights = jnp.where(allowed, jnp.exp(scores - new_top[:, :, :, None]), 0.0)
            shrink = jnp.exp(running_top - new_top)
            running_sum = running_sum * shrink + jnp.sum(weights, axis=3)
            running_out = running_out * shrink[:, :, :, None] + jnp.einsum(
                "sqhk,skhd->sqhd",
                weights.astype(jnp.bfloat16),
                value_block,
                preferred_element_type=jnp.float32,
            )
            return (new_top, running_sum, running_out)

        def unchanged(inner_state):
            return inner_state

        return (lax.cond(key_start <= last_position, compute, unchanged, block_state), None)

    result, unused = lax.scan(one_block, start_state, jnp.arange(key_total // block_rows))
    final_top, final_sum, final_out = result
    attn_out = (
        (final_out / final_sum[:, :, :, None])
        .astype(jnp.bfloat16)
        .reshape(seq_count, token_count, attn_cols)
    )
    pool_flat = jnp.transpose(
        pool_out.reshape(seq_count, tp_count, own_count, pool_cols), (1, 0, 2, 3)
    ).reshape(tp_count * seq_count * own_count, pool_cols)
    attn_flat = jnp.transpose(
        attn_out.reshape(seq_count, tp_count, own_count, attn_cols), (1, 0, 2, 3)
    ).reshape(tp_count * seq_count * own_count, attn_cols)
    summed = lax.psum_scatter(
        (
            jnp.dot(pool_flat, out_pool_full, preferred_element_type=jnp.float32)
            + jnp.dot(attn_flat, out_attn_full, preferred_element_type=jnp.float32)
        ).astype(jnp.bfloat16),
        "tp",
        scatter_dimension=0,
        tiled=True,
    ).astype(jnp.float32)
    return summed.astype(jnp.bfloat16).reshape(seq_count, own_count, summed.shape[1])


query_block = 512
log2_e = 1.4426950408889634


def attention_kernel(*refs):
    *part_refs, column_ref, row_ref, out_ref, packed_ref = refs
    block = pl.program_id(0)
    place = lax.axis_index("sp")
    part_count = len(part_refs)
    part_rows = part_refs[0].shape[0]

    @pl.when(block == 0)
    def fill():
        for by, part_ref in enumerate(part_refs):
            source = lax.rem(place + part_count - by, part_count)
            at = pl.multiple_of(source * part_rows, part_rows)
            packed_ref[pl.ds(at, part_rows), :] = part_ref[...]

    gate = column_ref[...]

    def scored(start, low, high):
        scores = lax.dot_general(
            packed_ref[start : start + query_block, 0:HEAD_DIM],
            packed_ref[low:high, HEAD_DIM : 2 * HEAD_DIM],
            (((1,), (1,)), ((), ())),
            preferred_element_type=jnp.float32,
        )
        return scores * (HEAD_DIM ** (-0.5) * log2_e) + (gate - row_ref[:, low:high])

    def weighted(scores, top, low, high):
        lifted = jnp.exp2(scores - top)
        values = packed_ref[low:high, 2 * HEAD_DIM : 3 * HEAD_DIM]
        return jnp.sum(lifted, axis=1, keepdims=True), jnp.dot(
            lifted.astype(jnp.bfloat16), values, preferred_element_type=jnp.float32
        )

    def visit(start):
        end = start + query_block
        last = scored(start, start, end)
        below = lax.broadcasted_iota(jnp.int32, last.shape, 1) <= lax.broadcasted_iota(
            jnp.int32, last.shape, 0
        )
        last = jnp.where(below, last, masked_score)
        top = jnp.max(last, axis=1, keepdims=True)
        if start > 0:
            before = scored(start, 0, start)
            top = jnp.maximum(top, jnp.max(before, axis=1, keepdims=True))
        denominator, total = weighted(last, top, start, end)
        if start > 0:
            more_sum, more_total = weighted(before, top, 0, start)
            denominator = denominator + more_sum
            total = total + more_total
        out_ref[...] = (total / denominator).astype(jnp.bfloat16)

    for index in range(packed_ref.shape[0] // query_block):
        pl.when(block == index)(lambda index=index: visit(index * query_block))


def attend(parts, gate):
    rows = sum(part.shape[0] for part in parts)
    gate = gate * log2_e
    return pl.pallas_call(
        attention_kernel,
        grid=(rows // query_block,),
        in_specs=[
            *[pl.BlockSpec(part.shape, lambda i: (0, 0)) for part in parts],
            pl.BlockSpec((query_block, 1), lambda i: (i, 0)),
            pl.BlockSpec((1, rows), lambda i: (0, 0)),
        ],
        out_specs=pl.BlockSpec((query_block, HEAD_DIM), lambda i: (i, 0)),
        out_shape=jax.ShapeDtypeStruct((rows, HEAD_DIM), jnp.bfloat16),
        scratch_shapes=[
            pltpu.VMEM((rows, 3 * HEAD_DIM), jnp.bfloat16),
        ],
        cost_estimate=pl.CostEstimate(
            flops=2 * rows * rows * HEAD_DIM * 2,
            bytes_accessed=rows * HEAD_DIM * 8,
            transcendentals=rows * rows // 2,
        ),
        compiler_params=pltpu.CompilerParams(vmem_limit_bytes=32 * 1024 * 1024),
    )(*parts, gate[:, None], gate[None, :])


def over_fs(own):
    def flip(x, bit):
        return lax.ppermute(x, "fs", [(i, i ^ bit) for i in range(4)])

    sibling = flip(own, 1)
    across = flip(own, 2)
    corner = flip(across, 1)
    return jnp.concatenate([own, sibling, across, corner], axis=0)


def swap(x):
    return lax.ppermute(x, "tp", [(0, 1), (1, 0)])


def around(x, by):
    length = lax.axis_size("sp")
    return lax.ppermute(x, "sp", [(i, (i + by) % length) for i in range(length)])


def fast_device(
    tokens,
    norm_gain,
    w_pool_in,
    pool_mix,
    pool_scale,
    w_query,
    w_key,
    w_value,
    gate_cache,
    w_out_pool,
    w_out_attn,
):
    tp_index = lax.axis_index("tp")
    sp_index = lax.axis_index("sp")
    fs_index = lax.axis_index("fs")
    sp_count = lax.axis_size("sp")
    seq_count, own_count, width = tokens.shape
    token_count = 2 * own_count
    first_position = sp_index * token_count
    pool_cols = w_pool_in.shape[1]
    attn_cols = w_query.shape[1]
    group_local = pool_cols // GROUP_WIDTH
    others = [swap(tokens[s]) for s in range(seq_count)]
    query_full, key_full, value_full, pool_full = (
        over_fs(weight) for weight in (w_query, w_key, w_value, w_pool_in)
    )
    out_own = jnp.concatenate([w_out_pool, w_out_attn], axis=0)
    out_own, pool_full, value_full = lax.optimization_barrier((out_own, pool_full, value_full))
    out_all = (
        lax.all_gather(out_own, "fs", axis=0, tiled=False),
        lax.all_gather(swap(out_own), "fs", axis=0, tiled=False),
    )
    mixing = lax.dynamic_slice_in_dim(pool_mix, tp_index * group_local, group_local, 0)
    scaling = lax.dynamic_slice_in_dim(pool_scale, tp_index * pool_cols, pool_cols, 0)
    gates = lax.dynamic_index_in_dim(gate_cache, sp_index, 1, keepdims=False)

    def normalize(x):
        rows = x.astype(jnp.float32)
        return (
            rows
            * lax.rsqrt(jnp.mean(rows * rows, axis=-1, keepdims=True) + norm_eps)
            * norm_gain[None, :]
        ).astype(jnp.bfloat16)

    def project(rows, weights):
        return jnp.dot(rows, weights, preferred_element_type=jnp.float32).astype(jnp.bfloat16)

    arrived = []
    pooled = []
    for s in range(seq_count):
        mine = tokens[s]
        rows = normalize(
            jnp.concatenate(
                [
                    jnp.where(tp_index == 0, mine, others[s]),
                    jnp.where(tp_index == 0, others[s], mine),
                ],
                axis=0,
            )
        )
        depth = w_query.shape[0]
        rows = jnp.concatenate(
            [
                lax.dynamic_slice_in_dim(rows, jnp.bitwise_xor(fs_index, mask) * depth, depth, 1)
                for mask in range(4)
            ],
            axis=1,
        )
        heads = [project(rows, full) for full in (query_full, key_full, value_full)]

        def message(dest):
            at = dest * HEAD_DIM
            return jnp.concatenate(
                [
                    lax.dynamic_slice_in_dim(item, at, HEAD_DIM, 1) for item in heads
                ],
                axis=1,
            )

        parts = []
        for by in range(sp_count):
            part = message((sp_index + by) % sp_count)
            parts.append(around(part, by) if by > 0 else part)
        arrived.append(parts)
        pool_in = project(rows, pool_full)
        border = shifted(pool_in[token_count - (widest - 1) :], "sp", 1)
        pooled.append(
            pool_branch(
                pool_in, border, tp_index * group_local, first_position, mixing, scaling
            )
        )

    outputs = []
    for s in range(seq_count):
        attn = attend(arrived[s], gates[s])
        gathered = jnp.zeros((token_count, attn_cols), jnp.bfloat16)
        for by in range(sp_count):
            dest = (sp_index + by) % sp_count
            part = lax.dynamic_slice_in_dim(attn, dest * token_count, token_count, 0)
            if by > 0:
                part = around(part, by)
            gathered = lax.dynamic_update_slice_in_dim(
                gathered, part, ((sp_index + sp_count - by) % sp_count) * HEAD_DIM, 1
            )

        def halves(x):
            own = lax.dynamic_slice_in_dim(x, tp_index * own_count, own_count, 0)
            return own, swap(
                lax.dynamic_slice_in_dim(x, (1 - tp_index) * own_count, own_count, 0)
            )

        pool_own, pool_other = halves(pooled[s])
        attn_own, attn_other = halves(gathered)
        result = jnp.einsum(
            "mk,fkn->mfn",
            jnp.concatenate([pool_own, attn_own], axis=1),
            out_all[0],
            preferred_element_type=jnp.float32,
        ) + jnp.einsum(
            "mk,fkn->mfn",
            jnp.concatenate([pool_other, attn_other], axis=1),
            out_all[1],
            preferred_element_type=jnp.float32,
        )
        outputs.append(result.astype(jnp.bfloat16).reshape(own_count, width))
    return jnp.stack(outputs, axis=0)


def on_device(*args):
    heads = args[5].shape[1] // HEAD_DIM
    sp_count = lax.axis_size("sp")
    suited = lax.axis_size("tp") == 2 and lax.axis_size("fs") == 4 and heads == sp_count
    length = args[0].shape[1] * 2 * sp_count
    if suited and length % query_block == 0:
        return fast_device(*args)
    return general_device(*args)


def solution(mesh):
    placed = (
        P("fs", ("sp", "tp"), None),
        P(),
        P("fs", "tp"),
        P(),
        P(),
        P("fs", "tp"),
        P("fs", "tp"),
        P("fs", "tp"),
        P("fs", "tp", None),
        P("tp", "fs"),
        P("tp", "fs"),
    )
    return jax.shard_map(
        on_device,
        mesh=mesh,
        in_specs=placed,
        out_specs=P("fs", ("sp", "tp"), None),
        check_vma=False,
    )
```
